32 devices in a mesh: ep: 8 (over z, core), tp: 4 (over y, x).
Axes of the slice: x: 2, y: 2, z: 4, core: 2. Of those that a mesh axis runs over, the one named last changes fastest.
Arguments:
- tokens: bfloat16 [1024, 2048], P('ep', 'tp'), may hold values from -540 to 540
- expert_ids: int32 [1024, 2], P('ep'), may hold values from 0 to 7, all different within a row; in each aligned block of 128 rows (0 to 127, 128 to 255, ...) at most 64 rows name the same one
- gate_weights: float32 [1024, 2], P('ep'), may hold values from 0.1 to 1
- gain_in: float32 [2048], P('tp'), may hold values from 0.1 to 1.9
- gain_out: float32 [2048], P('tp'), may hold values from 0.1 to 1.9
- w_gate: bfloat16 [8, 2048, 8192], P('ep', None, 'tp'), may hold values from -0.125 to 0.125
- w_up: bfloat16 [8, 2048, 8192], P('ep', None, 'tp'), may hold values from -0.125 to 0.125
- w_down: bfloat16 [8, 8192, 2048], P('ep', 'tp'), may hold values from -0.397747564 to 0.397747564
Outputs:
- mixed: bfloat16 [1024, 2048], P('ep', 'tp')
The draws below stay inside these ranges and needn't reach their ends.
Inputs may be any that keep to these rules, and one draw needn't show every extreme that they name: `expert_ids`: each row names 2 different experts. In the rows of one index of ep (aligned blocks of 128 rows) no expert is named by more than 64 rows, a bound that some block reaches.
All inputs are finite; a program needn't handle non-finite values.
Results may differ from the reference program's by a relative error of at most 0.018.
Values may be sent and summed in bfloat16 or wider, within the bound.
A program may use at most 64 MiB of HBM per device.

```python
import math
import jax
import jax.numpy as jnp
import numpy as np
from jax import lax

D = 2048
FF = 8192
TOP = 2
TOK_DEV = 128
EXPERTS = 8
CAP = 64
TOKENS = 1024
N_EP = 8
N_TP = 4


def draw_tokens(key, part):
    keys = jax.random.split(jax.random.fold_in(key, 11), 3)
    rough = jnp.exp(jax.random.uniform(keys[0], (D,), jnp.float32, -0.4, 0.4))
    row_scale = jnp.exp(jax.random.uniform(keys[1], (TOKENS, 1), jnp.float32, 0.0, math.log(10.0)))
    rising = jnp.exp(jnp.linspace(0.0, math.log(6.0), D)).astype(jnp.float32)
    base = jax.random.normal(keys[2], (TOKENS, D), jnp.float32)
    base = jnp.clip(base, -6.0, 6.0)
    return (base * rough[None, :] * rising[None, :] * row_scale).astype(jnp.bfloat16)


def draw_w_down(key, part):
    keys = jax.random.split(jax.random.fold_in(key, 23), 2)
    rough = jnp.exp(jax.random.uniform(keys[0], (D,), jnp.float32, -0.4, 0.4))
    rising = jnp.exp(jnp.linspace(0.0, math.log(4.0), D)).astype(jnp.float32)
    base = jax.random.normal(keys[1], (EXPERTS, FF, D), jnp.float32)
    base = jnp.clip(base, -6.0, 6.0) / math.sqrt(FF)
    return (base * rough[None, None, :] * rising[None, None, :]).astype(jnp.bfloat16)


def levels(stream_key, extent, cuts, low, top_value):
    level = 1.0
    for position, shards_of in cuts:
        draws = jax.random.uniform(jax.random.fold_in(jax.random.fold_in(stream_key, 6), position), (shards_of,), jnp.float32, low / len(cuts), top_value / len(cuts))
        level = level * jnp.repeat(jnp.exp(draws), extent[position] // shards_of).reshape((-1,) + (1,) * (len(extent) - 1 - position))
    return level


def shared_out(key, own, number, rows, amount, top, limit, lean):
    ranking = jax.random.permutation(key, amount)
    heavy_load, ordinary = load_shares(amount, rows * top, limit, lean, True), load_shares(amount, rows * top, limit, lean, False)
    places = jnp.arange(amount)

    def named(sizes, rotation):
        used = int((sizes > 0).sum())
        fixed = max(1, used // 4)
        shifted = fixed + (places - fixed + rotation * (used - fixed)) % max(1, amount - fixed)
        return jnp.zeros((amount,), jnp.int32).at[ranking[jnp.where(places < fixed, places, shifted)]].set(jnp.asarray(sizes, jnp.int32))

    sizes = jnp.where(number % 4 == 0, named(heavy_load, number // 4), named(ordinary, number - number // 4 - 1))
    mixed = jax.random.permutation(jax.random.fold_in(own, 3), amount)
    donor, sink = mixed[0:amount // 2 * 2:2], mixed[1:amount // 2 * 2:2]
    margin = jnp.minimum(sizes[donor] - 1, limit - sizes[sink]) // 2
    margin = jnp.where((donor == ranking[0]) | (sink == ranking[0]) | (sizes[sink] == 0), 0, jnp.maximum(margin, 0))
    shifted = jax.random.randint(jax.random.fold_in(own, 4), (amount // 2,), 0, 1 << 20) % (margin + 1)
    sizes = sizes.at[donor].add(-shifted).at[sink].add(shifted)
    members = jnp.searchsorted(jnp.cumsum(sizes), jnp.arange(rows * top), side="right").astype(jnp.int32)
    table = members.reshape(top, rows).T
    table = table[jax.random.permutation(jax.random.fold_in(own, 1), rows)]
    rotation = jax.random.randint(jax.random.fold_in(own, 2), (rows, 1), 0, top)
    return jnp.take_along_axis(table, (jnp.arange(top)[None, :] + rotation) % top, axis=1)


def load_shares(number_of, total, limit, skew, full):
    loads = [(1 << 20) // math.isqrt(rank ** skew) + 1 for rank in range(1, number_of + 1)]
    largest = limit if full else min(limit, max(-(-total // number_of), total * loads[0] // sum(loads)))
    least = 1 if total - largest >= number_of - 1 else 0
    counts, spare = [largest] + [least] * (number_of - 1), total - largest - least * (number_of - 1)
    while spare > 0:
        candidates = [i for i in range(1, number_of) if counts[i] < largest] or [i for i in range(1, number_of) if counts[i] < limit]
        pool, budget = sum([loads[i] for i in candidates]), spare
        for i in candidates:
            extra = min(limit - counts[i], max(1, budget * loads[i] // pool), spare)
            counts[i] = counts[i] + extra
            spare = spare - extra
    return np.array(counts)


def scatter_about(rng, dims, scale, most, pieces=(), held_as=jnp.bfloat16):
    level = levels(rng, dims, pieces, -0.22, 0.18) if pieces else 1.0
    values = jax.random.normal(rng, dims, jnp.float32) * scale * level
    return jnp.minimum(jnp.maximum(values, -most), most).astype(held_as)


def setup_inputs(seed: int = 0) -> dict:
    key_of = jax.random.split(jax.random.key(seed), 9)
    tokens = draw_tokens(jax.random.fold_in(key_of[8], 71), 0)
    expert_ids_keys = jax.random.split(jax.random.fold_in(key_of[1], 1), TOKENS // TOK_DEV)
    expert_ids_turns = jax.random.permutation(jax.random.fold_in(key_of[1], 3), TOKENS // TOK_DEV)
    expert_ids = jax.vmap(lambda own, number: shared_out(jax.random.fold_in(key_of[1], 2), own, number, TOK_DEV, EXPERTS, TOP, CAP, 2))(expert_ids_keys, expert_ids_turns).reshape((TOKENS, TOP))
    gate_weights = jnp.clip(0.1 + 0.9 * jax.random.uniform(key_of[2], (TOKENS, TOP), jnp.float32) ** levels(key_of[2], (TOKENS, TOP), ((0, 8),), -0.2, 0.2), 0.1, 1.0)
    gain_in = jnp.clip(1.0 + 0.18 * jax.random.normal(key_of[3], (D,), jnp.float32), 0.1, 1.9)
    gain_out = jnp.clip(1.0 + 0.18 * jax.random.normal(key_of[4], (D,), jnp.float32), 0.1, 1.9)
    w_gate = scatter_about(key_of[5], (EXPERTS, D, FF), D ** -0.5, 0.125, ((0, 8), (2, 4)))
    w_up = scatter_about(key_of[6], (EXPERTS, D, FF), D ** -0.5, 0.125, ((0, 8), (2, 4)))
    w_down = draw_w_down(jax.random.fold_in(key_of[8], 71), 0)
    return dict(tokens=tokens, expert_ids=expert_ids, gate_weights=gate_weights, gain_in=gain_in, gain_out=gain_out, w_gate=w_gate, w_up=w_up, w_down=w_down)


NORM_EPS = 1e-06

def reference(tokens, expert_ids, gate_weights, gain_in, gain_out, w_gate, w_up, w_down):
    values = tokens.astype(jnp.float32)
    normed = (values * lax.rsqrt(lax.optimization_barrier(jnp.mean(values * values, axis=-1, keepdims=True)) + NORM_EPS) * gain_in).astype(jnp.bfloat16)
    grouped = expert_ids.reshape(N_EP, TOK_DEV * TOP)
    one_hot = (grouped[:, :, None] == jnp.arange(EXPERTS, dtype=jnp.int32)[None, None, :]).astype(jnp.int32)
    earlier = jnp.cumsum(one_hot, axis=1) - 1
    slot_index = lax.optimization_barrier(jnp.sum(one_hot * earlier, axis=-1))
    source_dev = jnp.arange(N_EP, dtype=jnp.int32)[:, None]
    row_place = (grouped * (N_EP * CAP) + source_dev * CAP + slot_index).reshape(-1).astype(jnp.int32)
    token_of = jnp.repeat(jnp.arange(TOKENS, dtype=jnp.int32), TOP)
    buffer = jnp.zeros((EXPERTS * N_EP * CAP, D), jnp.bfloat16).at[row_place].set(normed[token_of])
    buffer = buffer.reshape(EXPERTS, N_EP * CAP, D)
    slice_width = FF // N_TP

    def expert(operands):
        expert_rows, gate_w, up_w, down_w = operands
        gate_part = jnp.dot(expert_rows, gate_w, preferred_element_type=jnp.float32)
        up_part = jnp.dot(expert_rows, up_w, preferred_element_type=jnp.float32)
        hidden = (jax.nn.silu(gate_part) * up_part).astype(jnp.bfloat16)

        def add_slice(step, running):
            hidden_cols = lax.dynamic_slice_in_dim(hidden, step * slice_width, slice_width, 1)
            down_rows = lax.dynamic_slice_in_dim(down_w, step * slice_width, slice_width, 0)
            partial_value = jnp.dot(hidden_cols, down_rows, preferred_element_type=jnp.float32).astype(jnp.bfloat16)
            partial_value = lax.optimization_barrier(partial_value)
            return running + partial_value.astype(jnp.float32)
        return lax.fori_loop(0, N_TP, add_slice, jnp.zeros((N_EP * CAP, D), jnp.float32))
    outputs = lax.map(expert, (buffer, w_gate, w_up, w_down)).reshape(EXPERTS * N_EP * CAP, D)
    picked = outputs[row_place].reshape(TOKENS, TOP, D)
    combined = lax.optimization_barrier(jnp.sum(gate_weights[:, :, None] * picked, axis=1))
    scale = lax.rsqrt(lax.optimization_barrier(jnp.mean(combined * combined, axis=-1, keepdims=True)) + NORM_EPS)
    return (combined * scale * gain_out).astype(jnp.bfloat16)
```

```python
import jax
import jax.numpy as jnp
from jax import lax
from jax.experimental import pallas as pl
from jax.experimental.pallas import tpu as pltpu
from jax.sharding import PartitionSpec as P

TOP = 2


NORM_EPS = 1e-06


def on_device_plain(tokens, expert_ids, gate_weights, gain_in, gain_out, w_gate, w_up, w_down):
    count_tp = lax.axis_size("tp")
    count_ep = lax.axis_size("ep")
    tok_rows = tokens.shape[0]
    model_width = tokens.shape[1] * count_tp
    capacity = 2 * TOP * tok_rows // count_ep
    values = tokens.astype(jnp.float32)
    squares = lax.psum(jnp.sum(values * values, axis=1), "tp")
    normed = (values * lax.rsqrt(squares[:, None] / model_width + NORM_EPS) * gain_in).astype(
        jnp.bfloat16
    )
    flat_ids = expert_ids.reshape(-1)
    one_hot = (flat_ids[:, None] == jnp.arange(count_ep, dtype=jnp.int32)[None, :]).astype(
        jnp.int32
    )
    earlier = jnp.cumsum(one_hot, axis=0) - 1
    slot_index = jnp.sum(one_hot * earlier, axis=1)
    places = (flat_ids * capacity + slot_index).reshape(tok_rows, TOP)
    slot_rows = jnp.arange(count_ep * capacity, dtype=jnp.int32)
    picker = jnp.sum((slot_rows[:, None, None] == places[None, :, :]).astype(jnp.bfloat16), axis=2)
    gate_w = w_gate[0]
    up_w = w_up[0]
    down_w = w_down[0]
    outgoing = jnp.dot(picker, normed, preferred_element_type=jnp.float32).astype(jnp.bfloat16)
    arrived = lax.all_to_all(outgoing, "ep", split_axis=0, concat_axis=0, tiled=True)
    shard_part = lax.all_gather(arrived, "tp", axis=1, tiled=True)
    gate_part = jnp.dot(shard_part, gate_w, preferred_element_type=jnp.float32)
    up_part = jnp.dot(shard_part, up_w, preferred_element_type=jnp.float32)
    hidden = (jax.nn.silu(gate_part) * up_part).astype(jnp.bfloat16)
    partial_value = lax.optimization_barrier(
        jnp.dot(hidden, down_w, preferred_element_type=jnp.float32).astype(jnp.bfloat16)
    )
    summed = lax.psum_scatter(
        partial_value.astype(jnp.float32).astype(jnp.bfloat16),
        "tp",
        scatter_dimension=1,
        tiled=True,
    ).astype(jnp.float32)
    returned = lax.all_to_all(
        summed.astype(jnp.bfloat16), "ep", split_axis=0, concat_axis=0, tiled=True
    ).astype(summed.dtype)
    combined = jnp.sum(gate_weights[:, :, None] * returned[places], axis=1)
    squares_out = lax.psum(jnp.sum(combined * combined, axis=1), "tp")
    scale = lax.rsqrt(squares_out[:, None] / model_width + NORM_EPS)
    return (combined * scale * gain_out).astype(jnp.bfloat16)


MESH = pl.DeviceIdType.MESH


def greet_everyone(count, me, count_tp):
    barrier = pltpu.get_barrier_semaphore()

    @pl.loop(1, count)
    def _(step):
        peer = lax.rem(me + step, count)
        pl.semaphore_signal(
            barrier, inc=1, device_id=(peer // count_tp, lax.rem(peer, count_tp)),
            device_id_type=MESH,
        )

    pl.semaphore_wait(barrier, count - 1)


def dispatch_kernel(
    count_ep, count_tp, picked, gain, rows_out, gain_out,
    send_sem, recv_sem, gain_send, gain_recv, own_sem,
):
    ep, tp = lax.axis_index("ep"), lax.axis_index("tp")
    me, count = ep * count_tp + tp, count_ep * count_tp
    cap, width = picked.shape[1], picked.shape[2]

    def spot(owner):
        place_rows = pl.ds(pl.multiple_of((owner // count_tp) * cap, cap), cap)
        place_cols = pl.ds(pl.multiple_of(lax.rem(owner, count_tp) * width, width), width)
        return rows_out.at[place_rows, place_cols]

    def gain_spot(owner_tp):
        return gain_out.at[:, pl.ds(pl.multiple_of(owner_tp * width, width), width)]

    def rows_copy(peer, owner):
        return pltpu.make_async_remote_copy(
            src_ref=picked.at[peer // count_tp],
            dst_ref=spot(owner),
            send_sem=send_sem.at[peer],
            recv_sem=recv_sem.at[owner],
            device_id=(peer // count_tp, lax.rem(peer, count_tp)),
            device_id_type=MESH,
        )

    def gain_copy(peer_tp, owner_tp):
        return pltpu.make_async_remote_copy(
            src_ref=gain,
            dst_ref=gain_spot(owner_tp),
            send_sem=gain_send.at[peer_tp],
            recv_sem=gain_recv.at[owner_tp],
            device_id=(ep, peer_tp),
            device_id_type=MESH,
        )

    own_rows = pltpu.make_async_copy(picked.at[ep], spot(me), own_sem.at[0])
    own_gain = pltpu.make_async_copy(gain, gain_spot(tp), own_sem.at[1])
    own_rows.start()
    own_gain.start()
    greet_everyone(count, me, count_tp)

    @pl.loop(1, count)
    def _(step):
        rows_copy(lax.rem(me + step, count), me).start()

    for step in range(1, count_tp):
        gain_copy(lax.rem(tp + step, count_tp), tp).start()
    own_rows.wait()
    own_gain.wait()

    @pl.loop(1, count)
    def _(step):
        peer = lax.rem(me + step, count)
        copy = rows_copy(peer, peer)
        copy.wait_send()
        copy.wait_recv()

    for step in range(1, count_tp):
        peer_tp = lax.rem(tp + step, count_tp)
        copy = gain_copy(peer_tp, peer_tp)
        copy.wait_send()
        copy.wait_recv()


def dispatch(count_ep, count_tp, picked, gain):
    cap, width = picked.shape[1:]
    count = count_ep * count_tp
    return pl.pallas_call(
        lambda *refs: dispatch_kernel(count_ep, count_tp, *refs),
        out_shape=(
            jax.ShapeDtypeStruct((count_ep * cap, count_tp * width), picked.dtype),
            jax.ShapeDtypeStruct((gain.shape[0], count_tp * width), gain.dtype),
        ),
        in_specs=[pl.BlockSpec(memory_space=pltpu.VMEM)] * 2,
        out_specs=[pl.BlockSpec(memory_space=pltpu.VMEM)] * 2,
        scratch_shapes=[
            pltpu.SemaphoreType.DMA((count,)),
            pltpu.SemaphoreType.DMA((count,)),
            pltpu.SemaphoreType.DMA((count_tp,)),
            pltpu.SemaphoreType.DMA((count_tp,)),
            pltpu.SemaphoreType.DMA((2,)),
        ],
        compiler_params=pltpu.CompilerParams(collective_id=0, has_side_effects=True),
    )(picked, gain)


def return_kernel(
    count_ep, count_tp, partial, first_pick, second_pick, weights, gain, mixed,
    landed, stats, send_sem, recv_sem, stat_send, stat_recv, own_sem,
):
    ep, tp = lax.axis_index("ep"), lax.axis_index("tp")
    me, count = ep * count_tp + tp, count_ep * count_tp
    cap, width = partial.shape[0] // count_ep, partial.shape[1] // count_tp

    def source(owner):
        from_rows = pl.ds(pl.multiple_of((owner // count_tp) * cap, cap), cap)
        from_cols = pl.ds(pl.multiple_of(lax.rem(owner, count_tp) * width, width), width)
        return partial.at[from_rows, from_cols]

    def spot(owner):
        place_rows = pl.ds(pl.multiple_of((owner // count_tp) * cap, cap), cap)
        return landed.at[lax.rem(owner, count_tp), place_rows, :]

    def rows_copy(peer, owner):
        return pltpu.make_async_remote_copy(
            src_ref=source(peer),
            dst_ref=spot(owner),
            send_sem=send_sem.at[peer],
            recv_sem=recv_sem.at[owner],
            device_id=(peer // count_tp, lax.rem(peer, count_tp)),
            device_id_type=MESH,
        )

    def stat_copy(peer_tp, owner_tp):
        return pltpu.make_async_remote_copy(
            src_ref=stats.at[tp],
            dst_ref=stats.at[owner_tp],
            send_sem=stat_send.at[peer_tp],
            recv_sem=stat_recv.at[owner_tp],
            device_id=(ep, peer_tp),
            device_id_type=MESH,
        )

    own_rows = pltpu.make_async_copy(source(me), spot(me), own_sem.at[0])
    own_rows.start()
    greet_everyone(count, me, count_tp)

    @pl.loop(1, count)
    def _(step):
        rows_copy(lax.rem(me + step, count), me).start()

    own_rows.wait()

    @pl.loop(1, count)
    def _(step):
        peer = lax.rem(me + step, count)
        copy = rows_copy(peer, peer)
        copy.wait_send()
        copy.wait_recv()

    def picked_sum(pick):
        total = jnp.zeros(mixed.shape, jnp.float32)
        for part in range(count_tp):
            total += jnp.dot(pick[...], landed[part], preferred_element_type=jnp.float32)
        return total

    combined = weights[:, 0:1] * picked_sum(first_pick) + weights[:, 1:2] * picked_sum(second_pick)
    squares = jnp.sum(combined * combined, axis=1, keepdims=True)
    stats[tp] = jnp.broadcast_to(squares, stats.shape[1:])
    for step in range(1, count_tp):
        stat_copy(lax.rem(tp + step, count_tp), tp).start()
    for step in range(1, count_tp):
        peer_tp = lax.rem(tp + step, count_tp)
        copy = stat_copy(peer_tp, peer_tp)
        copy.wait_send()
        copy.wait_recv()
    everything = stats[0]
    for part in range(1, count_tp):
        everything += stats[part]
    scale = lax.rsqrt(everything[:, 0:1] / (count_tp * width) + NORM_EPS)
    mixed[...] = (combined * scale * gain[...]).astype(mixed.dtype)


def give_back(count_ep, count_tp, partial, picks, weights, gain):
    tok_rows, width = weights.shape[0], gain.shape[1]
    count = count_ep * count_tp
    return pl.pallas_call(
        lambda *refs: return_kernel(count_ep, count_tp, *refs),
        out_shape=jax.ShapeDtypeStruct((tok_rows, width), jnp.bfloat16),
        in_specs=[pl.BlockSpec(memory_space=pltpu.VMEM)] * 5,
        out_specs=pl.BlockSpec(memory_space=pltpu.VMEM),
        scratch_shapes=[
            pltpu.VMEM((count_tp, partial.shape[0], width), jnp.bfloat16),
            pltpu.VMEM((count_tp, tok_rows, 128), jnp.float32),
            pltpu.SemaphoreType.DMA((count,)),
            pltpu.SemaphoreType.DMA((count,)),
            pltpu.SemaphoreType.DMA((count_tp,)),
            pltpu.SemaphoreType.DMA((count_tp,)),
            pltpu.SemaphoreType.DMA((1,)),
        ],
        compiler_params=pltpu.CompilerParams(collective_id=1, has_side_effects=True),
    )(partial, picks[0], picks[1], weights, gain)


def on_device_direct(
    tokens, expert_ids, gate_weights, gain_in, gain_out, w_gate, w_up, w_down
):
    count_tp = lax.axis_size("tp")
    count_ep = lax.axis_size("ep")
    tok_rows, width = tokens.shape
    model_width = width * count_tp
    capacity = 2 * TOP * tok_rows // count_ep
    flat_ids = expert_ids.reshape(-1)
    experts = jnp.arange(count_ep, dtype=jnp.int32)
    named = (expert_ids[:, :, None] == experts).astype(jnp.float32)
    per_token = jnp.sum(named, axis=1)
    positions = jnp.arange(tok_rows, dtype=jnp.int32)
    before = (positions[:, None] > positions[None, :]).astype(jnp.float32)
    earlier = jnp.dot(before, per_token, preferred_element_type=jnp.float32)
    slot_index = jnp.sum(named * earlier[:, None, :], axis=2).astype(jnp.int32)
    places = expert_ids * capacity + slot_index
    slot_rows = jnp.arange(count_ep * capacity, dtype=jnp.int32)
    picks = [
        (places[:, k : k + 1] == slot_rows[None, :]).astype(jnp.bfloat16) for k in range(TOP)
    ]
    picker = (
        (slot_rows[:, None] == places[None, :, 0]) | (slot_rows[:, None] == places[None, :, 1])
    ).astype(jnp.bfloat16)
    picked = jnp.dot(picker, tokens, preferred_element_type=jnp.float32).astype(jnp.bfloat16)
    rows, gain = dispatch(
        count_ep, count_tp, picked.reshape(count_ep, capacity, width),
        jnp.broadcast_to(gain_in[None, :], (8, width)),
    )
    values = rows.astype(jnp.float32)
    squares = jnp.sum(values * values, axis=1, keepdims=True)
    normed = (values * lax.rsqrt(squares / model_width + NORM_EPS) * gain[0:1]).astype(
        jnp.bfloat16
    )
    gate_part = jnp.dot(normed, w_gate[0], preferred_element_type=jnp.float32)
    up_part = jnp.dot(normed, w_up[0], preferred_element_type=jnp.float32)
    hidden = (jax.nn.silu(gate_part) * up_part).astype(jnp.bfloat16)
    partial = jnp.dot(hidden, w_down[0], preferred_element_type=jnp.float32).astype(jnp.bfloat16)
    return give_back(count_ep, count_tp, partial, picks, gate_weights, gain_out[None, :])


def on_device(tokens, *others):
    if tokens.shape[1] % 128:
        return on_device_plain(tokens, *others)
    return on_device_direct(tokens, *others)


def solution(mesh):
    placed = (
        P("ep", "tp"),
        P("ep", None),
        P("ep", None),
        P("tp"),
        P("tp"),
        P("ep", None, "tp"),
        P("ep", None, "tp"),
        P("ep", "tp", None),
    )
    return jax.shard_map(
        on_device, mesh=mesh, in_specs=placed, out_specs=P("ep", "tp"), check_vma=False
    )
```

```python
import jax
import jax.numpy as jnp
from jax import lax
from jax.experimental import pallas as pl
from jax.experimental.pallas import tpu as pltpu
from jax.sharding import PartitionSpec as P

TOP = 2


NORM_EPS = 1e-06


def on_device_plain(tokens, expert_ids, gate_weights, gain_in, gain_out, w_gate, w_up, w_down):
    count_tp = lax.axis_size("tp")
    count_ep = lax.axis_size("ep")
    tok_rows = tokens.shape[0]
    model_width = tokens.shape[1] * count_tp
    capacity = 2 * TOP * tok_rows // count_ep
    values = tokens.astype(jnp.float32)
    squares = lax.psum(jnp.sum(values * values, axis=1), "tp")
    normed = (values * lax.rsqrt(squares[:, None] / model_width + NORM_EPS) * gain_in).astype(
        jnp.bfloat16
    )
    flat_ids = expert_ids.reshape(-1)
    one_hot = (flat_ids[:, None] == jnp.arange(count_ep, dtype=jnp.int32)[None, :]).astype(
        jnp.int32
    )
    earlier = jnp.cumsum(one_hot, axis=0) - 1
    slot_index = jnp.sum(one_hot * earlier, axis=1)
    places = (flat_ids * capacity + slot_index).reshape(tok_rows, TOP)
    slot_rows = jnp.arange(count_ep * capacity, dtype=jnp.int32)
    picker = jnp.sum((slot_rows[:, None, None] == places[None, :, :]).astype(jnp.bfloat16), axis=2)
    gate_w = w_gate[0]
    up_w = w_up[0]
    down_w = w_down[0]
    outgoing = jnp.dot(picker, normed, preferred_element_type=jnp.float32).astype(jnp.bfloat16)
    arrived = lax.all_to_all(outgoing, "ep", split_axis=0, concat_axis=0, tiled=True)
    shard_part = lax.all_gather(arrived, "tp", axis=1, tiled=True)
    gate_part = jnp.dot(shard_part, gate_w, preferred_element_type=jnp.float32)
    up_part = jnp.dot(shard_part, up_w, preferred_element_type=jnp.float32)
    hidden = (jax.nn.silu(gate_part) * up_part).astype(jnp.bfloat16)
    partial_value = lax.optimization_barrier(
        jnp.dot(hidden, down_w, preferred_element_type=jnp.float32).astype(jnp.bfloat16)
    )
    summed = lax.psum_scatter(
        partial_value.astype(jnp.float32).astype(jnp.bfloat16),
        "tp",
        scatter_dimension=1,
        tiled=True,
    ).astype(jnp.float32)
    returned = lax.all_to_all(
        summed.astype(jnp.bfloat16), "ep", split_axis=0, concat_axis=0, tiled=True
    ).astype(summed.dtype)
    combined = jnp.sum(gate_weights[:, :, None] * returned[places], axis=1)
    squares_out = lax.psum(jnp.sum(combined * combined, axis=1), "tp")
    scale = lax.rsqrt(squares_out[:, None] / model_width + NORM_EPS)
    return (combined * scale * gain_out).astype(jnp.bfloat16)


MESH = pl.DeviceIdType.MESH


def greet(count_ep, count_tp, ep, tp):
    barrier = pltpu.get_barrier_semaphore()
    for step in range(1, count_ep):
        peer = (lax.rem(ep + step, count_ep), tp)
        pl.semaphore_signal(barrier, inc=1, device_id=peer, device_id_type=MESH)
    for step in range(1, count_tp):
        peer = (ep, lax.rem(tp + step, count_tp))
        pl.semaphore_signal(barrier, inc=1, device_id=peer, device_id_type=MESH)
    pl.semaphore_wait(barrier, count_ep + count_tp - 2)


def dispatch_kernel(
    count_ep, count_tp, picked, gain, rows_out, gain_out,
    send_sem, recv_sem, pass_send, pass_recv, gain_send, gain_recv, own_sem,
):
    ep, tp = lax.axis_index("ep"), lax.axis_index("tp")
    cap, width = picked.shape[1], picked.shape[2]

    def spot(owner, owner_tp):
        place_rows = pl.ds(pl.multiple_of(owner * cap, cap), cap)
        place_cols = pl.ds(pl.multiple_of(owner_tp * width, width), width)
        return rows_out.at[place_rows, place_cols]

    def gain_spot(owner_tp):
        return gain_out.at[:, pl.ds(pl.multiple_of(owner_tp * width, width), width)]

    def rows_copy(peer, owner):
        return pltpu.make_async_remote_copy(
            src_ref=picked.at[peer],
            dst_ref=spot(owner, tp),
            send_sem=send_sem.at[peer],
            recv_sem=recv_sem.at[owner],
            device_id=(peer, tp),
            device_id_type=MESH,
        )

    def pass_copy(source, block, peer_tp, owner_tp):
        return pltpu.make_async_remote_copy(
            src_ref=source,
            dst_ref=spot(block, owner_tp),
            send_sem=pass_send.at[block, peer_tp],
            recv_sem=pass_recv.at[block, owner_tp],
            device_id=(ep, peer_tp),
            device_id_type=MESH,
        )

    def gain_copy(peer_tp, owner_tp):
        return pltpu.make_async_remote_copy(
            src_ref=gain,
            dst_ref=gain_spot(owner_tp),
            send_sem=gain_send.at[peer_tp],
            recv_sem=gain_recv.at[owner_tp],
            device_id=(ep, peer_tp),
            device_id_type=MESH,
        )

    own_rows = pltpu.make_async_copy(picked.at[ep], spot(ep, tp), own_sem.at[0])
    own_gain = pltpu.make_async_copy(gain, gain_spot(tp), own_sem.at[1])
    own_rows.start()
    own_gain.start()
    greet(count_ep, count_tp, ep, tp)
    for step in range(1, count_ep):
        rows_copy(lax.rem(ep + step, count_ep), ep).start()
    for step in range(1, count_tp):
        peer_tp = lax.rem(tp + step, count_tp)
        pass_copy(picked.at[ep], ep, peer_tp, tp).start()
        gain_copy(peer_tp, tp).start()
    own_rows.wait()
    own_gain.wait()

    @pl.loop(1, count_ep)
    def _(step):
        block = lax.rem(ep + count_ep - step, count_ep)
        rows_copy(block, block).wait_recv()
        for hop in range(1, count_tp):
            peer_tp = lax.rem(tp + hop, count_tp)
            pass_copy(spot(block, tp), block, peer_tp, tp).start()

    for step in range(1, count_ep):
        peer = lax.rem(ep + step, count_ep)
        rows_copy(peer, peer).wait_send()

    @pl.loop(0, count_ep)
    def _(step):
        block = lax.rem(ep + count_ep - step, count_ep)
        for hop in range(1, count_tp):
            peer_tp = lax.rem(tp + hop, count_tp)
            copy = pass_copy(spot(block, tp), block, peer_tp, peer_tp)
            copy.wait_send()
            copy.wait_recv()

    for step in range(1, count_tp):
        peer_tp = lax.rem(tp + step, count_tp)
        copy = gain_copy(peer_tp, peer_tp)
        copy.wait_send()
        copy.wait_recv()


def dispatch(count_ep, count_tp, picked, gain):
    cap, width = picked.shape[1:]
    return pl.pallas_call(
        lambda *refs: dispatch_kernel(count_ep, count_tp, *refs),
        out_shape=(
            jax.ShapeDtypeStruct((count_ep * cap, count_tp * width), picked.dtype),
            jax.ShapeDtypeStruct((gain.shape[0], count_tp * width), gain.dtype),
        ),
        in_specs=[pl.BlockSpec(memory_space=pltpu.VMEM)] * 2,
        out_specs=[pl.BlockSpec(memory_space=pltpu.VMEM)] * 2,
        scratch_shapes=[
            pltpu.SemaphoreType.DMA((count_ep,)),
            pltpu.SemaphoreType.DMA((count_ep,)),
            pltpu.SemaphoreType.DMA((count_ep, count_tp)),
            pltpu.SemaphoreType.DMA((count_ep, count_tp)),
            pltpu.SemaphoreType.DMA((count_tp,)),
            pltpu.SemaphoreType.DMA((count_tp,)),
            pltpu.SemaphoreType.DMA((2,)),
        ],
        compiler_params=pltpu.CompilerParams(collective_id=0, has_side_effects=True),
    )(picked, gain)


def return_kernel(
    count_ep, count_tp, partial, first_pick, second_pick, weights, gain, mixed,
    landed, summed, back, stats,
    send_sem, recv_sem, part_send, part_recv, stat_send, stat_recv,
):
    ep, tp = lax.axis_index("ep"), lax.axis_index("tp")
    cap, width = partial.shape[0] // count_ep, partial.shape[1] // count_tp

    def block_rows(block):
        return pl.ds(pl.multiple_of(block * cap, cap), cap)

    def part_cols(part):
        return pl.ds(pl.multiple_of(part * width, width), width)

    def part_copy(block, peer_tp, owner_tp):
        return pltpu.make_async_remote_copy(
            src_ref=partial.at[block_rows(block), part_cols(peer_tp)],
            dst_ref=landed.at[owner_tp, block_rows(block), :],
            send_sem=part_send.at[block, peer_tp],
            recv_sem=part_recv.at[block, owner_tp],
            device_id=(ep, peer_tp),
            device_id_type=MESH,
        )

    def back_copy(peer, owner):
        return pltpu.make_async_remote_copy(
            src_ref=summed.at[block_rows(peer), :],
            dst_ref=back.at[block_rows(owner), :],
            send_sem=send_sem.at[peer],
            recv_sem=recv_sem.at[owner],
            device_id=(peer, tp),
            device_id_type=MESH,
        )

    def stat_copy(peer_tp, owner_tp):
        return pltpu.make_async_remote_copy(
            src_ref=stats.at[tp],
            dst_ref=stats.at[owner_tp],
            send_sem=stat_send.at[peer_tp],
            recv_sem=stat_recv.at[owner_tp],
            device_id=(ep, peer_tp),
            device_id_type=MESH,
        )

    def block_sum(block):
        total = partial[block_rows(block), part_cols(tp)].astype(jnp.float32)
        for hop in range(1, count_tp):
            peer_tp = lax.rem(tp + hop, count_tp)
            part_copy(block, peer_tp, peer_tp).wait_recv()
            total += landed[peer_tp, block_rows(block), :].astype(jnp.float32)
        return total.astype(jnp.bfloat16)

    greet(count_ep, count_tp, ep, tp)

    @pl.loop(1, count_ep + 1)
    def _(step):
        block = lax.rem(ep + step, count_ep)
        for hop in range(1, count_tp):
            part_copy(block, lax.rem(tp + hop, count_tp), tp).start()

    @pl.loop(1, count_ep)
    def _(step):
        block = lax.rem(ep + step, count_ep)
        summed[block_rows(block), :] = block_sum(block)
        back_copy(block, ep).start()

    back[block_rows(ep), :] = block_sum(ep)

    @pl.loop(1, count_ep)
    def _(step):
        peer = lax.rem(ep + count_ep - step, count_ep)
        copy = back_copy(peer, peer)
        copy.wait_send()
        copy.wait_recv()

    @pl.loop(0, count_ep)
    def _(block):
        for hop in range(1, count_tp):
            part_copy(block, lax.rem(tp + hop, count_tp), tp).wait_send()

    returned = back[...]
    combined = weights[:, 0:1] * jnp.dot(
        first_pick[...], returned, preferred_element_type=jnp.float32
    ) + weights[:, 1:2] * jnp.dot(
        second_pick[...], returned, preferred_element_type=jnp.float32
    )
    squares = jnp.sum(combined * combined, axis=1, keepdims=True)
    stats[tp] = jnp.broadcast_to(squares, stats.shape[1:])
    for step in range(1, count_tp):
        stat_copy(lax.rem(tp + step, count_tp), tp).start()
    for step in range(1, count_tp):
        peer_tp = lax.rem(tp + step, count_tp)
        copy = stat_copy(peer_tp, peer_tp)
        copy.wait_send()
        copy.wait_recv()
    everything = stats[0]
    for part in range(1, count_tp):
        everything += stats[part]
    scale = lax.rsqrt(everything[:, 0:1] / (count_tp * width) + NORM_EPS)
    mixed[...] = (combined * scale * gain[...]).astype(mixed.dtype)


def give_back(count_ep, count_tp, partial, picks, weights, gain):
    tok_rows, width = weights.shape[0], gain.shape[1]
    return pl.pallas_call(
        lambda *refs: return_kernel(count_ep, count_tp, *refs),
        out_shape=jax.ShapeDtypeStruct((tok_rows, width), jnp.bfloat16),
        in_specs=[pl.BlockSpec(memory_space=pltpu.VMEM)] * 5,
        out_specs=pl.BlockSpec(memory_space=pltpu.VMEM),
        scratch_shapes=[
            pltpu.VMEM((count_tp, partial.shape[0], width), jnp.bfloat16),
            pltpu.VMEM((partial.shape[0], width), jnp.bfloat16),
            pltpu.VMEM((partial.shape[0], width), jnp.bfloat16),
            pltpu.VMEM((count_tp, tok_rows, 128), jnp.float32),
            pltpu.SemaphoreType.DMA((count_ep,)),
            pltpu.SemaphoreType.DMA((count_ep,)),
            pltpu.SemaphoreType.DMA((count_ep, count_tp)),
            pltpu.SemaphoreType.DMA((count_ep, count_tp)),
            pltpu.SemaphoreType.DMA((count_tp,)),
            pltpu.SemaphoreType.DMA((count_tp,)),
        ],
        compiler_params=pltpu.CompilerParams(collective_id=1, has_side_effects=True),
    )(partial, picks[0], picks[1], weights, gain)


def on_device_direct(
    tokens, expert_ids, gate_weights, gain_in, gain_out, w_gate, w_up, w_down
):
    count_tp = lax.axis_size("tp")
    count_ep = lax.axis_size("ep")
    tok_rows, width = tokens.shape
    model_width = width * count_tp
    capacity = 2 * TOP * tok_rows // count_ep
    flat_ids = expert_ids.reshape(-1)
    experts = jnp.arange(count_ep, dtype=jnp.int32)
    named = (expert_ids[:, :, None] == experts).astype(jnp.float32)
    per_token = jnp.sum(named, axis=1)
    positions = jnp.arange(tok_rows, dtype=jnp.int32)
    before = (positions[:, None] > positions[None, :]).astype(jnp.float32)
    earlier = jnp.dot(before, per_token, preferred_element_type=jnp.float32)
    slot_index = jnp.sum(named * earlier[:, None, :], axis=2).astype(jnp.int32)
    places = expert_ids * capacity + slot_index
    slot_rows = jnp.arange(count_ep * capacity, dtype=jnp.int32)
    picks = [
        (places[:, k : k + 1] == slot_rows[None, :]).astype(jnp.bfloat16) for k in range(TOP)
    ]
    picker = (
        (slot_rows[:, None] == places[None, :, 0]) | (slot_rows[:, None] == places[None, :, 1])
    ).astype(jnp.bfloat16)
    picked = jnp.dot(picker, tokens, preferred_element_type=jnp.float32).astype(jnp.bfloat16)
    rows, gain = dispatch(
        count_ep, count_tp, picked.reshape(count_ep, capacity, width),
        jnp.broadcast_to(gain_in[None, :], (8, width)),
    )
    values = rows.astype(jnp.float32)
    squares = jnp.sum(values * values, axis=1, keepdims=True)
    normed = (values * lax.rsqrt(squares / model_width + NORM_EPS) * gain[0:1]).astype(
        jnp.bfloat16
    )
    gate_part = jnp.dot(normed, w_gate[0], preferred_element_type=jnp.float32)
    up_part = jnp.dot(normed, w_up[0], preferred_element_type=jnp.float32)
    hidden = (jax.nn.silu(gate_part) * up_part).astype(jnp.bfloat16)
    partial = jnp.dot(hidden, w_down[0], preferred_element_type=jnp.float32).astype(jnp.bfloat16)
    return give_back(count_ep, count_tp, partial, picks, gate_weights, gain_out[None, :])


def on_device(tokens, *others):
    if tokens.shape[1] % 128:
        return on_device_plain(tokens, *others)
    return on_device_direct(tokens, *others)


def solution(mesh):
    placed = (
        P("ep", "tp"),
        P("ep", None),
        P("ep", None),
        P("tp"),
        P("tp"),
        P("ep", None, "tp"),
        P("ep", None, "tp"),
        P("ep", "tp", None),
    )
    return jax.shard_map(
        on_device, mesh=mesh, in_specs=placed, out_specs=P("ep", "tp"), check_vma=False
    )
```
